256 devices in a mesh: grp: 2 (over y), fs: 16 (over z), tp: 8 (over x, core).
Axes of the slice: x: 4, y: 2, z: 16, core: 2. Of those that a mesh axis runs over, the one named last changes fastest.
The devices are a block of a 4x16x16 slice.
Arguments:
- tokens: bfloat16 [8192, 2048], P(('grp', 'tp')), parts along dimension 0, may hold values from -6 to 6
- gate_weight: float32 [2, 2048, 5632], P(None, 'fs', 'tp'), may hold values from -0.125 to 0.125
- up_weight: float32 [2, 2048, 5632], P(None, 'fs', 'tp'), may hold values from -0.125 to 0.125
- down_weight: float32 [2, 2048, 5632], P(None, 'fs', 'tp'), may hold values from -0.078125 to 0.078125
- in_gain: float32 [2, 2048], P(None, 'fs'), may hold values from 0.1 to 1.9
- out_gain: float32 [2, 2048], replicated, may hold values from 0.1 to 1.9
Outputs:
- sampler_gate: bfloat16 [4, 2048, 5632], P('grp', None, 'fs'), parts along dimension 0
- sampler_up: bfloat16 [4, 2048, 5632], P('grp', None, 'fs'), parts along dimension 0
- sampler_down: bfloat16 [4, 2048, 5632], P('grp', None, 'fs'), parts along dimension 0
- result: bfloat16 [8192, 2048], P(('grp', 'tp', 'fs')), parts along dimension 0
The draws below stay inside these ranges and needn't reach their ends.
There are 2 independent parts, one for each index of `grp`. The reference program is written for one: setup_inputs(seed, part) draws one part's arguments, and reference() takes and returns one part's arrays. A program takes and returns all parts, laid end to end along the dimension named above; an argument that names none is the same for every part. Nothing has to cross between parts.
All inputs are finite; a program needn't handle non-finite values.
Results may differ from the reference program's by a relative error of at most 0.0073.
Values may be sent and summed in bfloat16 or wider, within the bound.
No kernel may reach another device: no remote copies, remote signals or barrier semaphores. Data moves between devices by JAX's collectives and lax.ppermute only.
A program may use at most 128 MiB of HBM per device.

```python
import jax
import jax.numpy as jnp
from jax import lax

D = 2048
FF = 5632
TOKENS = 4096
HB = 44
N_FS = 16
N_TP = 8


def levels(stream_key, extent, shards, least, largest):
    loudness, own = 1.0, jax.random.fold_in(stream_key, 6)
    for position, shards_of in shards:
        draws = jnp.exp(jax.random.uniform(jax.random.fold_in(own, position), (shards_of,), jnp.float32, least / len(shards), largest / len(shards)))
        loudness = loudness * jnp.repeat(draws, extent[position] // shards_of).reshape([-1 if axis == position else 1 for axis in range(len(extent))])
    return loudness


def centred(stream_key, dims, width, bound, pieces=(), kind=jnp.bfloat16):
    entries = width * jax.random.normal(stream_key, dims, jnp.float32)
    if pieces:
        entries = entries * levels(stream_key, dims, pieces, -0.22, 0.18)
    return jnp.clip(entries, -bound, bound).astype(kind)


def setup_inputs(seed: int = 0, part: int = 0) -> dict:
    arg_keys = jax.random.split(jax.random.key(seed), 7)
    own_keys = jax.random.split(jax.random.fold_in(arg_keys[6], part), 7)
    return {
        "tokens": centred(own_keys[0], (TOKENS, D), 1.0, 6.0, ((0, 8),)),
        "gate_weight": centred(arg_keys[1], (2, D, FF), D ** -0.5, 0.125, ((1, 16), (2, 8)), jnp.float32),
        "up_weight": centred(arg_keys[2], (2, D, FF), D ** -0.5, 0.125, ((1, 16), (2, 8)), jnp.float32),
        "down_weight": centred(arg_keys[3], (2, D, FF), FF ** -0.5, 0.078125, ((1, 16), (2, 8)), jnp.float32),
        "in_gain": jnp.clip(1.0 + 0.18 * jax.random.normal(arg_keys[4], (2, D), jnp.float32), 0.1, 1.9),
        "out_gain": jnp.clip(1.0 + 0.18 * jax.random.normal(arg_keys[5], (2, D), jnp.float32), 0.1, 1.9),
    }


EPS = 1e-06

def normalize(rows):
    return rows * lax.rsqrt(lax.optimization_barrier(jnp.mean(rows * rows, axis=-1, keepdims=True)) + EPS)

def reorder(matrix):
    return matrix.reshape(D, N_TP, N_FS, HB).transpose(0, 2, 1, 3).reshape(D, FF)

def reference(tokens, gate_weight, up_weight, down_weight, in_gain, out_gain):
    gates = []
    ups = []
    downs = []
    state = tokens.astype(jnp.float32)
    rounded = tokens
    for section_idx in range(2):
        gate_matrix = (in_gain[section_idx][:, None] * gate_weight[section_idx]).astype(jnp.bfloat16)
        up_matrix = (in_gain[section_idx][:, None] * up_weight[section_idx]).astype(jnp.bfloat16)
        down_matrix = down_weight[section_idx].astype(jnp.bfloat16)
        gates.append(reorder(gate_matrix))
        ups.append(reorder(up_matrix))
        downs.append(reorder(down_matrix))
        normed = normalize(state).astype(jnp.bfloat16)
        gate_act = jnp.dot(normed, gate_matrix, preferred_element_type=jnp.float32)
        up_act = jnp.dot(normed, up_matrix, preferred_element_type=jnp.float32)
        hidden = (jax.nn.silu(gate_act) * up_act).astype(jnp.bfloat16)
        mixed = lax.dot_general(hidden, down_matrix, (((1,), (1,)), ((), ())), preferred_element_type=jnp.float32)
        rounded = lax.optimization_barrier((state + 0.5 * out_gain[section_idx] * normalize(mixed)).astype(jnp.bfloat16))
        state = rounded.astype(jnp.float32)
    return (jnp.stack(gates), jnp.stack(ups), jnp.stack(downs), rounded)
```

```python
import jax
import jax.numpy as jnp
from jax import lax
from jax.sharding import PartitionSpec as P

EPS = 1e-06


def shift(array, axis, by):
    n = lax.axis_size(axis)
    return lax.ppermute(array, axis, [(i, (i + by) % n) for i in range(n)])


def ring_sum(own, axis):
    n = lax.axis_size(axis)
    half = n // 2
    up = shift(own(half).astype(jnp.bfloat16), axis, 1)
    down = shift(own(half + 1).astype(jnp.bfloat16), axis, -1)
    for t in range(1, half):
        up = shift((up.astype(jnp.float32) + own(half - t)).astype(jnp.bfloat16), axis, 1)
        if t < half - 1:
            down = shift((down.astype(jnp.float32) + own(half + 1 + t)).astype(jnp.bfloat16), axis, -1)
    return up.astype(jnp.float32) + down.astype(jnp.float32) + own(0)


def ring_gather(rows, axis):
    n = lax.axis_size(axis)
    half = n // 2
    parts = [rows] + [None] * (n - 1)
    for t in range(1, half + 1):
        parts[n - t] = shift(parts[(n - t + 1) % n], axis, 1)
        if t < half:
            parts[t] = shift(parts[t - 1], axis, -1)
    return parts


def normalize(rows):
    return rows * lax.rsqrt(jnp.mean(rows * rows, axis=-1, keepdims=True) + EPS)


def body(tokens, gate_weight, up_weight, down_weight, in_gain, out_gain):
    groups = lax.axis_size("fs")
    columns = lax.axis_size("tp")
    here = lax.axis_index("fs")
    mine = tokens.shape[0] // groups
    width = tokens.shape[1]
    local_rows = gate_weight.shape[1]
    block = gate_weight.shape[2] // groups
    padded = -(-block // 16) * 16
    halves = (list(range(groups // 4 + 1, groups // 4 + 1 + groups // 2)),)
    first = halves[0]
    second = [k % groups for k in range(first[-1] + 1, first[-1] + 1 + groups // 2)]

    twice = jnp.concatenate([tokens, tokens], axis=0)
    rolled = lax.dynamic_slice_in_dim(twice, here * mine, tokens.shape[0], 0)
    residual = rolled[:mine].astype(jnp.float32)
    normed = normalize(rolled.astype(jnp.float32)).astype(jnp.bfloat16)
    parts = [normed[k * mine : (k + 1) * mine] for k in range(groups)]

    arrived = []
    for s in range(2):
        scale = in_gain[s][:, None]
        both = jnp.concatenate(
            [
                w.astype(jnp.bfloat16).T.reshape(groups, block, local_rows)
                for w in (scale * gate_weight[s], scale * up_weight[s], down_weight[s])
            ],
            axis=1,
        )
        got = lax.all_to_all(both, "fs", 0, 0, tiled=True)
        thin = [
            jnp.moveaxis(got[:, k * block : (k + 1) * block], 0, 1).reshape(block, width) for k in range(3)
        ]
        arrived.append(jnp.pad(jnp.concatenate(thin, axis=1), ((0, padded - block), (0, 0))))
    mats = [lax.all_gather(a, "tp", axis=0, tiled=False) for a in arrived]

    contract_last = (((1,), (1,)), ((), ()))
    outs = []
    state = None
    for s in range(2):
        flat = mats[s].reshape(columns * padded, 3 * width)
        gate, up, down = (flat[:, k * width : (k + 1) * width] for k in range(3))
        sums = [None] * groups
        for order in (first, second):
            rows = jnp.concatenate([parts[k] for k in order], axis=0)
            g = lax.dot_general(rows, gate, contract_last, preferred_element_type=jnp.float32)
            u = lax.dot_general(rows, up, contract_last, preferred_element_type=jnp.float32)
            hidden = (jax.nn.silu(g) * u).astype(jnp.bfloat16)
            part = jnp.dot(hidden, down, preferred_element_type=jnp.float32)
            for at, k in enumerate(order):
                sums[k] = part[at * mine : (at + 1) * mine]
        mixed = ring_sum(lambda k: sums[k], "fs")
        state = (residual + 0.5 * out_gain[s] * normalize(mixed)).astype(jnp.bfloat16)
        if s == 0:
            residual = state.astype(jnp.float32)
            parts = ring_gather(normalize(residual).astype(jnp.bfloat16), "fs")
        outs.append(
            [
                mats[s][:, :block, k * width : (k + 1) * width].reshape(columns * block, width).T
                for k in range(3)
            ]
        )
    return (*(jnp.stack([outs[s][k] for s in range(2)]) for k in range(3)), state)


def solution(mesh):
    in_specs = (
        P(("grp", "tp"), None),
        P(None, "fs", "tp"),
        P(None, "fs", "tp"),
        P(None, "fs", "tp"),
        P(None, "fs"),
        P(),
    )
    out_specs = (
        P("grp", None, "fs"),
        P("grp", None, "fs"),
        P("grp", None, "fs"),
        P(("grp", "tp", "fs"), None),
    )
    return jax.shard_map(body, mesh=mesh, in_specs=in_specs, out_specs=out_specs, check_vma=False)
```

```python
import jax
import jax.numpy as jnp
from jax import lax
from jax.experimental import pallas as pl
from jax.experimental.pallas import tpu as pltpu
from jax.sharding import PartitionSpec as P

EPS = 1e-06


def shift(array, axis, by):
    n = lax.axis_size(axis)
    return lax.ppermute(array, axis, [(i, (i + by) % n) for i in range(n)])


def ring_sum(own, axis):
    n = lax.axis_size(axis)
    half = n // 2
    up = shift(own(half), axis, 1)
    down = shift(own(half + 1), axis, -1)
    for t in range(1, half):
        up = shift((up.astype(jnp.float32) + own(half - t)).astype(jnp.bfloat16), axis, 1)
        if t < half - 1:
            down = shift((down.astype(jnp.float32) + own(half + 1 + t)).astype(jnp.bfloat16), axis, -1)
    return up.astype(jnp.float32) + down.astype(jnp.float32) + own(0).astype(jnp.float32)


def ring_gather(rows, axis):
    n = lax.axis_size(axis)
    half = n // 2
    parts = [rows] + [None] * (n - 1)
    for t in range(1, half + 1):
        parts[n - t] = shift(parts[(n - t + 1) % n], axis, 1)
        if t < half:
            parts[t] = shift(parts[t - 1], axis, -1)
    return parts


def select_kernel(kept, source, *refs):
    out = refs[-1]
    out[0] = lax.dot_general(
        source[...], kept[...], (((0,), (0,)), ((), ())), preferred_element_type=jnp.float32
    ).astype(jnp.bfloat16)


def turned(flat, kept, which, width, layer, layers, into):
    tile = 512
    units = kept.shape[1]
    steps = width // tile
    in_specs = [
        pl.BlockSpec(kept.shape, lambda t: (0, 0)),
        pl.BlockSpec((flat.shape[0], tile), lambda t: (0, which * steps + t)),
    ]
    operands = [kept, flat]
    aliases = {}
    if into is not None:
        in_specs.append(pl.BlockSpec(memory_space=pl.ANY))
        operands.append(into)
        aliases = {2: 0}
    return pl.pallas_call(
        select_kernel,
        out_shape=jax.ShapeDtypeStruct((layers, width, units), jnp.bfloat16),
        grid=(steps,),
        in_specs=in_specs,
        out_specs=pl.BlockSpec((1, tile, units), lambda t: (layer, t, 0)),
        input_output_aliases=aliases,
        cost_estimate=pl.CostEstimate(
            flops=2 * width * units * flat.shape[0],
            bytes_accessed=2 * width * (units + flat.shape[0]),
            transcendentals=0,
        ),
        compiler_params=pltpu.CompilerParams(vmem_limit_bytes=8 * 1024 * 1024),
        name="turned",
    )(*operands)


def normalize(rows):
    return rows * lax.rsqrt(jnp.mean(rows * rows, axis=-1, keepdims=True) + EPS)


def body(tokens, gate_weight, up_weight, down_weight, in_gain, out_gain):
    groups = lax.axis_size("fs")
    columns = lax.axis_size("tp")
    here = lax.axis_index("fs")
    mine = tokens.shape[0] // groups
    width = tokens.shape[1]
    local_rows = gate_weight.shape[1]
    block = gate_weight.shape[2] // groups
    padded = -(-block // 16) * 16
    halves = (list(range(groups // 4 + 1, groups // 4 + 1 + groups // 2)),)
    first = halves[0]
    second = [k % groups for k in range(first[-1] + 1, first[-1] + 1 + groups // 2)]

    twice = jnp.concatenate([tokens, tokens], axis=0)
    rolled = lax.dynamic_slice_in_dim(twice, here * mine, tokens.shape[0], 0)
    residual = rolled[:mine].astype(jnp.float32)
    normed = normalize(rolled.astype(jnp.float32)).astype(jnp.bfloat16)
    parts = [normed[k * mine : (k + 1) * mine] for k in range(groups)]

    arrived = []
    for s in range(2):
        scale = in_gain[s][:, None]
        both = jnp.concatenate(
            [
                w.astype(jnp.bfloat16).T.reshape(groups, block, local_rows)
                for w in (scale * gate_weight[s], scale * up_weight[s], down_weight[s])
            ],
            axis=1,
        )
        got = lax.all_to_all(both, "fs", 0, 0, tiled=True)
        thin = [
            jnp.moveaxis(got[:, k * block : (k + 1) * block], 0, 1).reshape(block, width) for k in range(3)
        ]
        arrived.append(jnp.pad(jnp.concatenate(thin, axis=1), ((0, padded - block), (0, 0))))
    mats = [lax.all_gather(a, "tp", axis=0, tiled=False) for a in arrived]

    contract_last = (((1,), (1,)), ((), ()))
    slot = jnp.arange(columns * padded)
    unit = jnp.where(slot % padded < block, slot // padded * block + slot % padded, -1)
    kept = (unit[:, None] == jnp.arange(columns * block)[None, :]).astype(jnp.bfloat16)
    outs = [None] * 3
    state = None
    for s in range(2):
        flat = mats[s].reshape(columns * padded, 3 * width)
        gate, up, down = (flat[:, k * width : (k + 1) * width] for k in range(3))
        sums = [None] * groups
        for order in (first, second):
            rows = jnp.concatenate([parts[k] for k in order], axis=0)
            g = lax.dot_general(rows, gate, contract_last, preferred_element_type=jnp.float32)
            u = lax.dot_general(rows, up, contract_last, preferred_element_type=jnp.float32)
            hidden = (jax.nn.silu(g) * u).astype(jnp.bfloat16)
            part = jnp.dot(hidden, down, preferred_element_type=jnp.float32).astype(jnp.bfloat16)
            for at, k in enumerate(order):
                sums[k] = part[at * mine : (at + 1) * mine]
        mixed = ring_sum(lambda k: sums[k], "fs")
        state = (residual + 0.5 * out_gain[s] * normalize(mixed)).astype(jnp.bfloat16)
        if s == 0:
            residual = state.astype(jnp.float32)
            parts = ring_gather(normalize(residual).astype(jnp.bfloat16), "fs")
        outs = [turned(flat, kept, k, width, s, 2, outs[k]) for k in range(3)]
    return (*outs, state)


def solution(mesh):
    in_specs = (
        P(("grp", "tp"), None),
        P(None, "fs", "tp"),
        P(None, "fs", "tp"),
        P(None, "fs", "tp"),
        P(None, "fs"),
        P(),
    )
    out_specs = (
        P("grp", None, "fs"),
        P("grp", None, "fs"),
        P("grp", None, "fs"),
        P(("grp", "tp", "fs"), None),
    )
    return jax.shard_map(body, mesh=mesh, in_specs=in_specs, out_specs=out_specs, check_vma=False)
```

```python
import functools

import jax
import jax.numpy as jnp
from jax import lax
from jax.experimental import pallas as pl
from jax.experimental.pallas import tpu as pltpu
from jax.sharding import PartitionSpec as P

EPS = 1e-06


def shift(array, axis, by):
    n = lax.axis_size(axis)
    return lax.ppermute(array, axis, [(i, (i + by) % n) for i in range(n)])


TILES = 8


def nothing_kernel(*outs):
    pass


def unwritten(shapes):
    return pl.pallas_call(
        nothing_kernel,
        out_shape=tuple(pltpu.HBM(s, jnp.bfloat16) for s in shapes),
        out_specs=(pl.BlockSpec(memory_space=pltpu.HBM),) * len(shapes),
        name="unwritten",
    )()


def place_kernel(layer, tile, kept, flat, a, b, c, out_a, out_b, out_c, source, result, arrive, leave):
    outs = (out_a, out_b, out_c)
    span = source.shape[2]

    def load(k):
        at = pl.multiple_of(k * span * TILES + tile[0] * span, span)
        return pltpu.make_async_copy(flat.at[:, pl.ds(at, span)], source.at[k], arrive.at[k])

    def store(k):
        at = pl.multiple_of(tile[0] * span, span)
        return pltpu.make_async_copy(result.at[k], outs[k].at[layer, :, pl.ds(at, span)], leave.at[k])

    for k in range(3):
        load(k).start()
    for k in range(3):
        load(k).wait()
        result[k] = jnp.dot(kept[...], source[k], preferred_element_type=jnp.float32).astype(jnp.bfloat16)
        store(k).start()
    for k in range(3):
        store(k).wait()


def place(outs, flat, kept, layer, tile):
    units, width = outs[0].shape[1:]
    slots, span = flat.shape[0], width // TILES
    whole = pl.BlockSpec(memory_space=pltpu.HBM)
    return pl.pallas_call(
        functools.partial(place_kernel, layer),
        out_shape=tuple(pltpu.HBM(o.shape, o.dtype) for o in outs),
        in_specs=[
            pl.BlockSpec(memory_space=pltpu.SMEM),
            pl.BlockSpec(memory_space=pltpu.VMEM),
            whole,
            whole,
            whole,
            whole,
        ],
        out_specs=(whole,) * 3,
        scratch_shapes=[
            pltpu.VMEM((3, slots, span), jnp.bfloat16),
            pltpu.VMEM((3, units, span), jnp.bfloat16),
            pltpu.SemaphoreType.DMA((3,)),
            pltpu.SemaphoreType.DMA((3,)),
        ],
        input_output_aliases={3: 0, 4: 1, 5: 2},
        cost_estimate=pl.CostEstimate(
            flops=6 * span * units * slots,
            bytes_accessed=6 * span * (units + slots),
            transcendentals=0,
        ),
        compiler_params=pltpu.CompilerParams(vmem_limit_bytes=4 * 1024 * 1024),
        name="place",
    )(jnp.full((1,), tile, jnp.int32), kept, flat, *outs)


def fold(carried, part):
    return (carried.astype(jnp.float32) + part.astype(jnp.float32)).astype(jnp.bfloat16)


def ring_sum(make, axis, work, beside):
    n = lax.axis_size(axis)
    half, quarter = n // 2, n // 4
    near = make(0)
    up = shift(near[quarter - 1], axis, 1)
    down = shift(near[quarter], axis, -1)
    far = make(1)
    up, down, far = lax.optimization_barrier((up, down, far))

    parts = jnp.concatenate([near, far], axis=0)

    def step(t, carry):
        up, down, work = carry
        a = lax.dynamic_index_in_dim(parts, (quarter - 1 - t) % n, 0, keepdims=False)
        b = lax.dynamic_index_in_dim(parts, quarter + t, 0, keepdims=False)
        work = beside(work, t - 1)
        return shift(fold(up, a), axis, 1), shift(fold(down, b), axis, -1), work

    up, down, work = lax.fori_loop(1, half - 1, step, (up, down, work))
    up = shift(fold(up, far[quarter]), axis, 1)
    for tile in range(half - 2, TILES):
        work = beside(work, tile)
    total = up.astype(jnp.float32) + down.astype(jnp.float32) + far[quarter - 1].astype(jnp.float32)
    return total, work


def ring_gather(rows, axis, work, beside):
    n = lax.axis_size(axis)
    half, own = n // 2, n - n // 4 - 1
    out = jnp.zeros((n, *rows.shape), rows.dtype)
    out = lax.dynamic_update_index_in_dim(out, rows, own, 0)

    def step(t, carry):
        up, down, out, work = carry
        next_up, next_down = shift(up, axis, 1), shift(down, axis, -1)
        work = beside(work, t - 1)
        out = lax.dynamic_update_index_in_dim(out, up, own - t, 0)
        out = lax.dynamic_update_index_in_dim(out, down, (own + t) % n, 0)
        return next_up, next_down, out, work

    first = (shift(rows, axis, 1), shift(rows, axis, -1), out, work)
    up, down, out, work = lax.fori_loop(1, half - 1, step, first)
    out = lax.dynamic_update_index_in_dim(out, up, own - half + 1, 0)
    out = lax.dynamic_update_index_in_dim(out, down, (own + half - 1) % n, 0)
    up = shift(up, axis, 1)
    for tile in range(half - 2, TILES):
        work = beside(work, tile)
    return lax.dynamic_update_index_in_dim(out, up, own - half, 0), work


def normalize(rows):
    return rows * lax.rsqrt(jnp.mean(rows * rows, axis=-1, keepdims=True) + EPS)


def body(tokens, gate_weight, up_weight, down_weight, in_gain, out_gain):
    groups = lax.axis_size("fs")
    columns = lax.axis_size("tp")
    here = lax.axis_index("fs")
    mine = tokens.shape[0] // groups
    width = tokens.shape[1]
    local_rows = gate_weight.shape[1]
    block = gate_weight.shape[2] // groups
    padded = -(-block // 16) * 16
    turn = groups // 4 + 1
    own = groups - turn

    twice = jnp.concatenate([tokens, tokens], axis=0)
    rolled = lax.dynamic_slice_in_dim(
        twice, (here + turn) % groups * mine, tokens.shape[0], 0
    )
    residual = rolled[own * mine : (own + 1) * mine].astype(jnp.float32)
    rows = normalize(rolled.astype(jnp.float32)).astype(jnp.bfloat16)

    arrived = []
    for s in range(2):
        scale = in_gain[s][:, None]
        both = jnp.concatenate(
            [
                w.astype(jnp.bfloat16).T.reshape(groups, block, local_rows)
                for w in (scale * gate_weight[s], scale * up_weight[s], down_weight[s])
            ],
            axis=1,
        )
        got = lax.all_to_all(both, "fs", 0, 0, tiled=True)
        thin = [
            jnp.moveaxis(got[:, k * block : (k + 1) * block], 0, 1).reshape(block, width) for k in range(3)
        ]
        arrived.append(jnp.pad(jnp.concatenate(thin, axis=1), ((0, padded - block), (0, 0))))
    mats = [lax.all_gather(a, "tp", axis=0, tiled=False) for a in arrived]

    contract_last = (((1,), (1,)), ((), ()))
    slot = jnp.arange(columns * padded)
    unit = jnp.where(slot % padded < block, slot // padded * block + slot % padded, -1)
    kept = (jnp.arange(columns * block)[:, None] == unit[None, :]).astype(jnp.bfloat16)
    outs = unwritten([(2, columns * block, width)] * 3)
    flats = [m.reshape(columns * padded, 3 * width) for m in mats]
    state = None
    for s in range(2):
        gate, up, down = (flats[s][:, k * width : (k + 1) * width] for k in range(3))

        def make(h):
            count = rows.shape[0] // 2
            some = rows[h * count : (h + 1) * count]
            g = lax.dot_general(some, gate, contract_last, preferred_element_type=jnp.float32)
            u = lax.dot_general(some, up, contract_last, preferred_element_type=jnp.float32)
            hidden = (jax.nn.silu(g) * u).astype(jnp.bfloat16)
            part = jnp.dot(hidden, down, preferred_element_type=jnp.float32).astype(jnp.bfloat16)
            return part.reshape(groups // 2, mine, width)

        if s == 0:
            mixed, _ = ring_sum(make, "fs", (), lambda work, tile: work)
        else:
            mixed, outs = ring_sum(make, "fs", outs, lambda work, tile: place(work, flats[1], kept, 1, tile))
        state = (residual + 0.5 * out_gain[s] * normalize(mixed)).astype(jnp.bfloat16)
        if s == 0:
            residual = state.astype(jnp.float32)
            rows, outs = ring_gather(
                normalize(residual).astype(jnp.bfloat16),
                "fs",
                outs,
                lambda work, tile: place(work, flats[0], kept, 0, tile),
            )
            rows = rows.reshape(tokens.shape)
    return (*(jnp.swapaxes(o, 1, 2) for o in outs), state)


def solution(mesh):
    in_specs = (
        P(("grp", "tp"), None),
        P(None, "fs", "tp"),
        P(None, "fs", "tp"),
        P(None, "fs", "tp"),
        P(None, "fs"),
        P(),
    )
    out_specs = (
        P("grp", None, "fs"),
        P("grp", None, "fs"),
        P("grp", None, "fs"),
        P(("grp", "tp", "fs"), None),
    )
    return jax.shard_map(body, mesh=mesh, in_specs=in_specs, out_specs=out_specs, check_vma=False)
```

```python
import functools

import jax
import jax.numpy as jnp
from jax import lax
from jax.experimental import pallas as pl
from jax.experimental.pallas import tpu as pltpu
from jax.sharding import PartitionSpec as P

EPS = 1e-06


def shift(array, axis, by):
    n = lax.axis_size(axis)
    return lax.ppermute(array, axis, [(i, (i + by) % n) for i in range(n)])


TILES = 8


def nothing_kernel(*outs):
    pass


def unwritten(shapes):
    return pl.pallas_call(
        nothing_kernel,
        out_shape=tuple(pltpu.HBM(s, jnp.bfloat16) for s in shapes),
        out_specs=(pl.BlockSpec(memory_space=pltpu.HBM),) * len(shapes),
        name="unwritten",
    )()


def place_kernel(layer, tile, kept, flat, a, b, c, out_a, out_b, out_c, source, result, arrive, leave):
    outs = (out_a, out_b, out_c)
    span = source.shape[2]

    def load(k):
        at = pl.multiple_of(k * span * TILES + tile[0] * span, span)
        return pltpu.make_async_copy(flat.at[:, pl.ds(at, span)], source.at[k], arrive.at[k])

    def store(k):
        at = pl.multiple_of(tile[0] * span, span)
        return pltpu.make_async_copy(result.at[k], outs[k].at[layer, :, pl.ds(at, span)], leave.at[k])

    for k in range(3):
        load(k).start()
    for k in range(3):
        load(k).wait()
        result[k] = jnp.dot(kept[...], source[k], preferred_element_type=jnp.float32).astype(jnp.bfloat16)
        store(k).start()
    for k in range(3):
        store(k).wait()


def place(outs, flat, kept, layer, tile):
    units, width = outs[0].shape[1:]
    slots, span = flat.shape[0], width // TILES
    whole = pl.BlockSpec(memory_space=pltpu.HBM)
    return pl.pallas_call(
        functools.partial(place_kernel, layer),
        out_shape=tuple(pltpu.HBM(o.shape, o.dtype) for o in outs),
        in_specs=[
            pl.BlockSpec(memory_space=pltpu.SMEM),
            pl.BlockSpec(memory_space=pltpu.VMEM),
            whole,
            whole,
            whole,
            whole,
        ],
        out_specs=(whole,) * 3,
        scratch_shapes=[
            pltpu.VMEM((3, slots, span), jnp.bfloat16),
            pltpu.VMEM((3, units, span), jnp.bfloat16),
            pltpu.SemaphoreType.DMA((3,)),
            pltpu.SemaphoreType.DMA((3,)),
        ],
        input_output_aliases={3: 0, 4: 1, 5: 2},
        cost_estimate=pl.CostEstimate(
            flops=6 * span * units * slots,
            bytes_accessed=6 * span * (units + slots),
            transcendentals=0,
        ),
        compiler_params=pltpu.CompilerParams(vmem_limit_bytes=4 * 1024 * 1024),
        name="place",
    )(jnp.full((1,), tile, jnp.int32), kept, flat, *outs)


def fold(carried, part):
    return (carried.astype(jnp.float32) + part.astype(jnp.float32)).astype(jnp.bfloat16)


def ring_sum(parts, axis, work, beside):
    n = lax.axis_size(axis)
    half = n // 2
    blank = jnp.zeros(parts.shape[1:], parts.dtype)

    def step(t, carry):
        up, down, _, work = carry
        a = lax.dynamic_index_in_dim(parts, half - t, 0, keepdims=False)
        b = lax.dynamic_index_in_dim(parts, jnp.minimum(half + 1 + t, n - 1), 0, keepdims=False)
        work = beside(work, t)
        return shift(fold(up, a), axis, 1), shift(fold(down, b), axis, -1), down, work

    up, _, down, work = lax.fori_loop(0, half, step, (blank, blank, blank, work))
    return up.astype(jnp.float32) + down.astype(jnp.float32) + parts[0].astype(jnp.float32), work


def ring_gather(rows, axis, work, beside):
    n = lax.axis_size(axis)
    half = n // 2
    out = lax.dynamic_update_index_in_dim(jnp.zeros((n, *rows.shape), rows.dtype), rows, 0, 0)

    def step(t, carry):
        up, down, out, work = carry
        up, down = shift(up, axis, 1), shift(down, axis, -1)
        work = beside(work, t)
        out = lax.dynamic_update_index_in_dim(out, up, n - 1 - t, 0)
        out = lax.dynamic_update_index_in_dim(out, down, t + 1, 0)
        return up, down, out, work

    _, _, out, work = lax.fori_loop(0, half, step, (rows, rows, out, work))
    return out, work


def partner(array, axis):
    return lax.ppermute(array, axis, [(i, i ^ 1) for i in range(lax.axis_size(axis))])


def same_core(mine, axis):
    return [mine] + [shift(mine, axis, by) for by in range(2, lax.axis_size(axis), 2)]


def both_cores(same, axis):
    return jnp.concatenate(same + [partner(piece, axis) for piece in same], axis=0)


def column_order(axis):
    n, here = lax.axis_size(axis), lax.axis_index(axis)
    back = jnp.arange(0, n, 2)
    return jnp.concatenate([(here - back) % n, ((here ^ 1) - back) % n])


def normalize(rows):
    return rows * lax.rsqrt(jnp.mean(rows * rows, axis=-1, keepdims=True) + EPS)


def body(tokens, gate_weight, up_weight, down_weight, in_gain, out_gain):
    groups = lax.axis_size("fs")
    columns = lax.axis_size("tp")
    here = lax.axis_index("fs")
    mine = tokens.shape[0] // groups
    width = tokens.shape[1]
    local_rows = gate_weight.shape[1]
    block = gate_weight.shape[2] // groups
    padded = -(-block // 16) * 16
    twice = jnp.concatenate([tokens, tokens], axis=0)
    rolled = lax.dynamic_slice_in_dim(twice, here * mine, tokens.shape[0], 0)
    residual = rolled[:mine].astype(jnp.float32)
    rows = normalize(rolled.astype(jnp.float32)).astype(jnp.bfloat16)

    got = []
    for s in range(2):
        scale = in_gain[s][:, None]
        both = jnp.concatenate(
            [
                w.astype(jnp.bfloat16).T.reshape(groups, block, local_rows)
                for w in (scale * gate_weight[s], scale * up_weight[s], down_weight[s])
            ],
            axis=1,
        )
        got.append(lax.all_to_all(both, "fs", 0, 0, tiled=True))

    def piece_of(arrived):
        thin = [
            jnp.moveaxis(arrived[:, k * block : (k + 1) * block], 0, 1).reshape(block, width) for k in range(3)
        ]
        return jnp.pad(jnp.concatenate(thin, axis=1), ((0, padded - block), (0, 0)))

    flats = [both_cores(same_core(piece_of(got[0]), "tp"), "tp"), None]

    contract_last = (((1,), (1,)), ((), ()))
    slot = jnp.arange(columns * padded)
    piece = jnp.repeat(column_order("tp"), padded)
    unit = jnp.where(slot % padded < block, piece * block + slot % padded, -1)
    kept = (jnp.arange(columns * block)[:, None] == unit[None, :]).astype(jnp.bfloat16)
    outs = unwritten([(2, columns * block, width)] * 3)
    state = None
    for s in range(2):
        gate, up, down = (flats[s][:, k * width : (k + 1) * width] for k in range(3))
        g = lax.dot_general(rows, gate, contract_last, preferred_element_type=jnp.float32)
        u = lax.dot_general(rows, up, contract_last, preferred_element_type=jnp.float32)
        hidden = (jax.nn.silu(g) * u).astype(jnp.bfloat16)
        part = jnp.dot(hidden, down, preferred_element_type=jnp.float32).astype(jnp.bfloat16)
        part = part.reshape(groups, mine, width)
        if s == 0:
            second, part = lax.optimization_barrier((got[1], part))
            same = same_core(piece_of(second), "tp")
            mixed, _ = ring_sum(part, "fs", (), lambda work, tile: work)
            mixed, same = lax.optimization_barrier((mixed, same))
            flats[1] = both_cores(same, "tp")
        else:
            mixed, outs = ring_sum(part, "fs", outs, lambda work, tile: place(work, flats[1], kept, 1, tile))
        state = (residual + 0.5 * out_gain[s] * normalize(mixed)).astype(jnp.bfloat16)
        if s == 0:
            residual = state.astype(jnp.float32)
            rows, outs = ring_gather(
                normalize(residual).astype(jnp.bfloat16),
                "fs",
                outs,
                lambda work, tile: place(work, flats[0], kept, 0, tile),
            )
            rows = rows.reshape(tokens.shape)
    return (*(jnp.swapaxes(o, 1, 2) for o in outs), state)


def solution(mesh):
    in_specs = (
        P(("grp", "tp"), None),
        P(None, "fs", "tp"),
        P(None, "fs", "tp"),
        P(None, "fs", "tp"),
        P(None, "fs"),
        P(),
    )
    out_specs = (
        P("grp", None, "fs"),
        P("grp", None, "fs"),
        P("grp", None, "fs"),
        P(("grp", "tp", "fs"), None),
    )
    return jax.shard_map(body, mesh=mesh, in_specs=in_specs, out_specs=out_specs, check_vma=False)
```

```python
import functools

import jax
import jax.numpy as jnp
from jax import lax
from jax.experimental import pallas as pl
from jax.experimental.pallas import tpu as pltpu
from jax.sharding import PartitionSpec as P

EPS = 1e-06


def shift(array, axis, by):
    n = lax.axis_size(axis)
    return lax.ppermute(array, axis, [(i, (i + by) % n) for i in range(n)])


TILES = 8


def nothing_kernel(*outs):
    pass


def unwritten(shapes):
    return pl.pallas_call(
        nothing_kernel,
        out_shape=tuple(pltpu.HBM(s, jnp.bfloat16) for s in shapes),
        out_specs=(pl.BlockSpec(memory_space=pltpu.HBM),) * len(shapes),
        name="unwritten",
    )()


def place_kernel(layer, tile, kept, flat, a, b, c, out_a, out_b, out_c, source, result, arrive, leave):
    outs = (out_a, out_b, out_c)
    span = source.shape[2]

    def load(k):
        at = pl.multiple_of(k * span * TILES + tile[0] * span, span)
        return pltpu.make_async_copy(flat.at[:, pl.ds(at, span)], source.at[k], arrive.at[k])

    def store(k):
        at = pl.multiple_of(tile[0] * span, span)
        return pltpu.make_async_copy(result.at[k], outs[k].at[layer, :, pl.ds(at, span)], leave.at[k])

    for k in range(3):
        load(k).start()
    for k in range(3):
        load(k).wait()
        result[k] = jnp.dot(kept[...], source[k], preferred_element_type=jnp.float32).astype(jnp.bfloat16)
        store(k).start()
    for k in range(3):
        store(k).wait()


def place(outs, flat, kept, layer, tile):
    units, width = outs[0].shape[1:]
    slots, span = flat.shape[0], width // TILES
    whole = pl.BlockSpec(memory_space=pltpu.HBM)
    return pl.pallas_call(
        functools.partial(place_kernel, layer),
        out_shape=tuple(pltpu.HBM(o.shape, o.dtype) for o in outs),
        in_specs=[
            pl.BlockSpec(memory_space=pltpu.SMEM),
            pl.BlockSpec(memory_space=pltpu.VMEM),
            whole,
            whole,
            whole,
            whole,
        ],
        out_specs=(whole,) * 3,
        scratch_shapes=[
            pltpu.VMEM((3, slots, span), jnp.bfloat16),
            pltpu.VMEM((3, units, span), jnp.bfloat16),
            pltpu.SemaphoreType.DMA((3,)),
            pltpu.SemaphoreType.DMA((3,)),
        ],
        input_output_aliases={3: 0, 4: 1, 5: 2},
        cost_estimate=pl.CostEstimate(
            flops=6 * span * units * slots,
            bytes_accessed=6 * span * (units + slots),
            transcendentals=0,
        ),
        compiler_params=pltpu.CompilerParams(vmem_limit_bytes=4 * 1024 * 1024),
        name="place",
    )(jnp.full((1,), tile, jnp.int32), kept, flat, *outs)


def fold(carried, part):
    return (carried.astype(jnp.float32) + part.astype(jnp.float32)).astype(jnp.bfloat16)


def ring_sum(parts, axis, work, beside):
    n = lax.axis_size(axis)
    half = n // 2
    up, down = shift(parts[half], axis, 1), shift(parts[half + 1], axis, -1)

    def step(t, carry):
        up, down, work = carry
        a = lax.dynamic_index_in_dim(parts, half - t, 0, keepdims=False)
        b = lax.dynamic_index_in_dim(parts, half + 1 + t, 0, keepdims=False)
        work = beside(work, t)
        return shift(fold(up, a), axis, 1), shift(fold(down, b), axis, -1), work

    up, down, work = lax.fori_loop(1, half - 1, step, (up, down, beside(work, 0)))
    up = shift(fold(up, parts[1]), axis, 1)
    work = beside(work, half - 1)
    return up.astype(jnp.float32) + down.astype(jnp.float32) + parts[0].astype(jnp.float32), work


def ring_gather(rows, axis, work, beside):
    n = lax.axis_size(axis)
    half = n // 2
    out = lax.dynamic_update_index_in_dim(jnp.zeros((n, *rows.shape), rows.dtype), rows, 0, 0)

    def step(t, carry):
        up, down, out, work = carry
        next_up, next_down = shift(up, axis, 1), shift(down, axis, -1)
        work = beside(work, t)
        out = lax.dynamic_update_index_in_dim(out, up, n - t, 0)
        out = lax.dynamic_update_index_in_dim(out, down, t, 0)
        return next_up, next_down, out, work

    first = (shift(rows, axis, 1), shift(rows, axis, -1), out, beside(work, 0))
    up, _, out, work = lax.fori_loop(1, half, step, first)
    return lax.dynamic_update_index_in_dim(out, up, half, 0), work


def partner(array, axis):
    return lax.ppermute(array, axis, [(i, i ^ 1) for i in range(lax.axis_size(axis))])


def same_core(mine, axis):
    return [mine] + [shift(mine, axis, by) for by in range(2, lax.axis_size(axis), 2)]


def both_cores(same, axis):
    return jnp.concatenate(same + [partner(piece, axis) for piece in same], axis=0)


def column_order(axis):
    n, here = lax.axis_size(axis), lax.axis_index(axis)
    back = jnp.arange(0, n, 2)
    return jnp.concatenate([(here - back) % n, ((here ^ 1) - back) % n])


def products_kernel(rows, flat, out):
    width = rows.shape[1]
    count = rows.shape[0] // 2
    last = (((1,), (1,)), ((), ()))
    for h in range(2):
        some = rows[h * count : (h + 1) * count]
        g = lax.dot_general(some, flat[:, :width], last, preferred_element_type=jnp.float32)
        u = lax.dot_general(some, flat[:, width : 2 * width], last, preferred_element_type=jnp.float32)
        hidden = (g / (1.0 + jnp.exp(-g)) * u).astype(jnp.bfloat16)
        part = jnp.dot(hidden, flat[:, 2 * width :], preferred_element_type=jnp.float32)
        out[h * count : (h + 1) * count] = part.astype(jnp.bfloat16)


def products(rows, flat):
    count, width = rows.shape
    return pl.pallas_call(
        products_kernel,
        out_shape=pltpu.VMEM((count, width), jnp.bfloat16),
        in_specs=[pl.BlockSpec(memory_space=pltpu.VMEM)] * 2,
        out_specs=pl.BlockSpec(memory_space=pltpu.VMEM),
        cost_estimate=pl.CostEstimate(
            flops=2 * count * flat.size, bytes_accessed=2 * (flat.size + 2 * rows.size), transcendentals=count * flat.shape[0]
        ),
        compiler_params=pltpu.CompilerParams(vmem_limit_bytes=30 * 1024 * 1024),
        name="products",
    )(rows, flat)


def normalize(rows):
    return rows * lax.rsqrt(jnp.mean(rows * rows, axis=-1, keepdims=True) + EPS)


def body(tokens, gate_weight, up_weight, down_weight, in_gain, out_gain):
    groups = lax.axis_size("fs")
    columns = lax.axis_size("tp")
    here = lax.axis_index("fs")
    mine = tokens.shape[0] // groups
    width = tokens.shape[1]
    local_rows = gate_weight.shape[1]
    block = gate_weight.shape[2] // groups
    padded = -(-block // 16) * 16
    twice = jnp.concatenate([tokens, tokens], axis=0)
    rolled = lax.dynamic_slice_in_dim(twice, here * mine, tokens.shape[0], 0)
    residual = rolled[:mine].astype(jnp.float32)
    rows = normalize(rolled.astype(jnp.float32)).astype(jnp.bfloat16)

    got = []
    for s in range(2):
        scale = in_gain[s][:, None]
        both = jnp.concatenate(
            [
                w.astype(jnp.bfloat16).T.reshape(groups, block, local_rows)
                for w in (scale * gate_weight[s], scale * up_weight[s], down_weight[s])
            ],
            axis=1,
        )
        got.append(lax.all_to_all(both, "fs", 0, 0, tiled=True))

    def piece_of(arrived):
        thin = [
            jnp.moveaxis(arrived[:, k * block : (k + 1) * block], 0, 1).reshape(block, width) for k in range(3)
        ]
        return jnp.pad(jnp.concatenate(thin, axis=1), ((0, padded - block), (0, 0)))

    flats = [both_cores(same_core(piece_of(got[0]), "tp"), "tp"), None]

    slot = jnp.arange(columns * padded)
    piece = jnp.repeat(column_order("tp"), padded)
    unit = jnp.where(slot % padded < block, piece * block + slot % padded, -1)
    kept = (jnp.arange(columns * block)[:, None] == unit[None, :]).astype(jnp.bfloat16)
    outs = unwritten([(2, columns * block, width)] * 3)
    state = None
    for s in range(2):
        part = products(rows, flats[s])
        part = part.reshape(groups, mine, width)
        if s == 0:
            mixed, _ = ring_sum(part, "fs", (), lambda work, tile: work)
        else:
            mixed, outs = ring_sum(part, "fs", outs, lambda work, tile: place(work, flats[1], kept, 1, tile))
        state = (residual + 0.5 * out_gain[s] * normalize(mixed)).astype(jnp.bfloat16)
        if s == 0:
            residual = state.astype(jnp.float32)
            second, residual = lax.optimization_barrier((got[1], residual))
            same = same_core(piece_of(second), "tp")
            rows, outs = ring_gather(
                normalize(residual).astype(jnp.bfloat16),
                "fs",
                outs,
                lambda work, tile: place(work, flats[0], kept, 0, tile),
            )
            rows, same = lax.optimization_barrier((rows.reshape(tokens.shape), same))
            flats[1] = both_cores(same, "tp")
    return (*(jnp.swapaxes(o, 1, 2) for o in outs), state)


def solution(mesh):
    in_specs = (
        P(("grp", "tp"), None),
        P(None, "fs", "tp"),
        P(None, "fs", "tp"),
        P(None, "fs", "tp"),
        P(None, "fs"),
        P(),
    )
    out_specs = (
        P("grp", None, "fs"),
        P("grp", None, "fs"),
        P("grp", None, "fs"),
        P(("grp", "tp", "fs"), None),
    )
    return jax.shard_map(body, mesh=mesh, in_specs=in_specs, out_specs=out_specs, check_vma=False)
```

```python
import functools

import jax
import jax.numpy as jnp
from jax import lax
from jax.experimental import pallas as pl
from jax.experimental.pallas import tpu as pltpu
from jax.sharding import PartitionSpec as P


EPS = 1e-06


def shift(array, axis, by):
    n = lax.axis_size(axis)
    return lax.ppermute(array, axis, [(i, (i + by) % n) for i in range(n)])


TILES = 8


def nothing_kernel(*outs):
    pass


def unwritten(shapes):
    return pl.pallas_call(
        nothing_kernel,
        out_shape=tuple(pltpu.HBM(s, jnp.bfloat16) for s in shapes),
        out_specs=(pl.BlockSpec(memory_space=pltpu.HBM),) * len(shapes),
        name="unwritten",
    )()


def place_kernel(layer, tile, kept, flat, a, b, c, out_a, out_b, out_c, source, result, arrive, leave):
    outs = (out_a, out_b, out_c)
    span = source.shape[2]

    def load(k):
        at = pl.multiple_of(k * span * TILES + tile[0] * span, span)
        return pltpu.make_async_copy(flat.at[:, pl.ds(at, span)], source.at[k], arrive.at[k])

    def store(k):
        at = pl.multiple_of(tile[0] * span, span)
        return pltpu.make_async_copy(result.at[k], outs[k].at[layer, :, pl.ds(at, span)], leave.at[k])

    for k in range(3):
        load(k).start()
    for k in range(3):
        load(k).wait()
        result[k] = jnp.dot(kept[...], source[k], preferred_element_type=jnp.float32).astype(jnp.bfloat16)
        store(k).start()
    for k in range(3):
        store(k).wait()


def place(outs, flat, kept, layer, tile):
    units, width = outs[0].shape[1:]
    slots, span = flat.shape[0], width // TILES
    whole = pl.BlockSpec(memory_space=pltpu.HBM)
    return pl.pallas_call(
        functools.partial(place_kernel, layer),
        out_shape=tuple(pltpu.HBM(o.shape, o.dtype) for o in outs),
        in_specs=[
            pl.BlockSpec(memory_space=pltpu.SMEM),
            pl.BlockSpec(memory_space=pltpu.VMEM),
            whole,
            whole,
            whole,
            whole,
        ],
        out_specs=(whole,) * 3,
        scratch_shapes=[
            pltpu.VMEM((3, slots, span), jnp.bfloat16),
            pltpu.VMEM((3, units, span), jnp.bfloat16),
            pltpu.SemaphoreType.DMA((3,)),
            pltpu.SemaphoreType.DMA((3,)),
        ],
        input_output_aliases={3: 0, 4: 1, 5: 2},
        cost_estimate=pl.CostEstimate(
            flops=6 * span * units * slots,
            bytes_accessed=6 * span * (units + slots),
            transcendentals=0,
        ),
        compiler_params=pltpu.CompilerParams(vmem_limit_bytes=4 * 1024 * 1024),
        name="place",
    )(jnp.full((1,), tile, jnp.int32), kept, flat, *outs)


def fold(carried, part):
    return (carried.astype(jnp.float32) + part.astype(jnp.float32)).astype(jnp.bfloat16)


def ring_sum(parts, axis, work, beside):
    n = lax.axis_size(axis)
    half = n // 2
    up, down = shift(parts[half], axis, 1), shift(parts[half + 1], axis, -1)

    def step(t, carry):
        up, down, work = carry
        a = lax.dynamic_index_in_dim(parts, half - t, 0, keepdims=False)
        b = lax.dynamic_index_in_dim(parts, half + 1 + t, 0, keepdims=False)
        work = beside(work, t)
        return shift(fold(up, a), axis, 1), shift(fold(down, b), axis, -1), work

    up, down, work = lax.fori_loop(1, half - 1, step, (up, down, beside(work, 0)))
    up = shift(fold(up, parts[1]), axis, 1)
    work = beside(work, half - 1)
    return up.astype(jnp.float32) + down.astype(jnp.float32) + parts[0].astype(jnp.float32), work


def open_kernel(rows, out):
    out[0] = rows[...]


def opened(rows, n):
    return pl.pallas_call(
        open_kernel,
        out_shape=pltpu.VMEM((n, *rows.shape), rows.dtype),
        in_specs=[pl.BlockSpec(memory_space=pltpu.VMEM)],
        out_specs=pl.BlockSpec(memory_space=pltpu.VMEM),
        compiler_params=pltpu.CompilerParams(vmem_limit_bytes=8 * 1024 * 1024),
        name="opened",
    )(rows)


def ring_gather(rows, axis, work, beside):
    n = lax.axis_size(axis)
    half = n // 2
    out = opened(rows, n)

    def step(t, carry):
        up, down, out, work = carry
        next_up, next_down = shift(up, axis, 1), shift(down, axis, -1)
        work = beside(work, t)
        out = lax.dynamic_update_index_in_dim(out, up, n - t, 0)
        out = lax.dynamic_update_index_in_dim(out, down, t, 0)
        return next_up, next_down, out, work

    first = (shift(rows, axis, 1), shift(rows, axis, -1), out, beside(work, 0))
    up, _, out, work = lax.fori_loop(1, half, step, first)
    return lax.dynamic_update_index_in_dim(out, up, half, 0), work


def partner(array, axis):
    return lax.ppermute(array, axis, [(i, i ^ 1) for i in range(lax.axis_size(axis))])


def same_core(mine, axis):
    return [mine] + [shift(mine, axis, by) for by in range(2, lax.axis_size(axis), 2)]


def both_cores(same, axis):
    return jnp.concatenate(same + [partner(piece, axis) for piece in same], axis=0)


def column_order(axis):
    n, here = lax.axis_size(axis), lax.axis_index(axis)
    back = jnp.arange(0, n, 2)
    return jnp.concatenate([(here - back) % n, ((here ^ 1) - back) % n])


def products_kernel(rows, flat, out):
    width = rows.shape[1]
    count = rows.shape[0] // 2
    last = (((1,), (1,)), ((), ()))
    for h in range(2):
        some = rows[h * count : (h + 1) * count]
        g = lax.dot_general(some, flat[:, :width], last, preferred_element_type=jnp.float32)
        u = lax.dot_general(some, flat[:, width : 2 * width], last, preferred_element_type=jnp.float32)
        hidden = (g / (1.0 + jnp.exp(-g)) * u).astype(jnp.bfloat16)
        part = jnp.dot(hidden, flat[:, 2 * width :], preferred_element_type=jnp.float32)
        out[h * count : (h + 1) * count] = part.astype(jnp.bfloat16)


def products(rows, flat):
    count, width = rows.shape
    return pl.pallas_call(
        products_kernel,
        out_shape=pltpu.VMEM((count, width), jnp.bfloat16),
        in_specs=[pl.BlockSpec(memory_space=pltpu.VMEM)] * 2,
        out_specs=pl.BlockSpec(memory_space=pltpu.VMEM),
        cost_estimate=pl.CostEstimate(
            flops=2 * count * flat.size, bytes_accessed=2 * (flat.size + 2 * rows.size), transcendentals=count * flat.shape[0]
        ),
        compiler_params=pltpu.CompilerParams(vmem_limit_bytes=30 * 1024 * 1024),
        name="products",
    )(rows, flat)


def normalize(rows):
    return rows * lax.rsqrt(jnp.mean(rows * rows, axis=-1, keepdims=True) + EPS)


def body(tokens, gate_weight, up_weight, down_weight, in_gain, out_gain):
    groups = lax.axis_size("fs")
    columns = lax.axis_size("tp")
    here = lax.axis_index("fs")
    mine = tokens.shape[0] // groups
    width = tokens.shape[1]
    local_rows = gate_weight.shape[1]
    block = gate_weight.shape[2] // groups
    padded = -(-block // 16) * 16
    twice = jnp.concatenate([tokens, tokens], axis=0)
    rolled = lax.dynamic_slice_in_dim(twice, here * mine, tokens.shape[0], 0)
    residual = rolled[:mine].astype(jnp.float32)
    rows = normalize(rolled.astype(jnp.float32)).astype(jnp.bfloat16)

    got = []
    for s in range(2):
        scale = in_gain[s][:, None]
        both = jnp.concatenate(
            [
                w.astype(jnp.bfloat16).T.reshape(groups, block, local_rows)
                for w in (scale * gate_weight[s], scale * up_weight[s], down_weight[s])
            ],
            axis=1,
        )
        got.append(lax.all_to_all(both, "fs", 0, 0, tiled=True))

    def piece_of(arrived):
        thin = [
            jnp.moveaxis(arrived[:, k * block : (k + 1) * block], 0, 1).reshape(block, width) for k in range(3)
        ]
        return jnp.pad(jnp.concatenate(thin, axis=1), ((0, padded - block), (0, 0)))

    first = piece_of(got[0])
    same = same_core(first, "tp")
    flats = [both_cores(same, "tp"), None]

    slot = jnp.arange(columns * padded)
    piece = jnp.repeat(column_order("tp"), padded)
    unit = jnp.where(slot % padded < block, piece * block + slot % padded, -1)
    kept = (jnp.arange(columns * block)[:, None] == unit[None, :]).astype(jnp.bfloat16)
    outs = unwritten([(2, columns * block, width)] * 3)
    state = None
    for s in range(2):
        part = products(rows, flats[s])
        part = part.reshape(groups, mine, width)
        if s == 0:
            mixed, _ = ring_sum(part, "fs", (), lambda work, tile: work)
        else:
            mixed, outs = ring_sum(part, "fs", outs, lambda work, tile: place(work, flats[1], kept, 1, tile))
        state = (residual + 0.5 * out_gain[s] * normalize(mixed)).astype(jnp.bfloat16)
        if s == 0:
            residual = state.astype(jnp.float32)
            second, residual = lax.optimization_barrier((got[1], residual))
            same = same_core(piece_of(second), "tp")
            rows, outs = ring_gather(
                normalize(residual).astype(jnp.bfloat16),
                "fs",
                outs,
                lambda work, tile: place(work, flats[0], kept, 0, tile),
            )
            rows, same = lax.optimization_barrier((rows.reshape(tokens.shape), same))
            flats[1] = both_cores(same, "tp")
    return (*(jnp.swapaxes(o, 1, 2) for o in outs), state)


def solution(mesh):
    in_specs = (
        P(("grp", "tp"), None),
        P(None, "fs", "tp"),
        P(None, "fs", "tp"),
        P(None, "fs", "tp"),
        P(None, "fs"),
        P(),
    )
    out_specs = (
        P("grp", None, "fs"),
        P("grp", None, "fs"),
        P("grp", None, "fs"),
        P(("grp", "tp", "fs"), None),
    )

    return jax.shard_map(body, mesh=mesh, in_specs=in_specs, out_specs=out_specs, check_vma=False)
```
